32 devices in a mesh: grp: 2 (over x), fs: 4 (over z), tp: 4 (over y, core).
Axes of the slice: x: 2, y: 2, z: 4, core: 2. Of those that a mesh axis runs over, the one named last changes fastest.
Arguments:
- tokens: bfloat16 [4096, 2048], P(('grp', 'fs')), parts along dimension 0, may hold values from -200 to 200
- norm_gain: float32 [2048], replicated, may hold values from 0.1 to 1.9
- value_weight: float32 [2048, 5632], P('fs', 'tp'), may hold values from -0.125 to 0.125
- gate_weight: float32 [2048, 5632], P('fs', 'tp'), may hold values from -0.125 to 0.125
- down_weight: float32 [2048, 5632], P('fs', 'tp'), may hold values from -0.078125 to 0.078125
- value_scale: float32 [5632], P('tp'), may hold values from 0.3 to 3
- gate_scale: float32 [5632], P('tp'), may hold values from 0.3 to 3
- down_scale: float32 [2048], replicated, may hold values from 0.3 to 3
- value_taps: float32 [3, 5632], P(None, 'tp'), may hold values from -3 to 3
- gate_taps: float32 [3, 5632], P(None, 'tp'), may hold values from -3 to 3
- value_bias: float32 [5632], P('tp'), may hold values from -3 to 3
- gate_bias: float32 [5632], P('tp'), may hold values from -3 to 3
Outputs:
- mixed: bfloat16 [4096, 2048], P(('grp', 'fs', 'tp')), parts along dimension 0
The draws below stay inside these ranges and needn't reach their ends.
There are 2 independent parts, one for each index of `grp`. The reference program is written for one: setup_inputs(seed, part) draws one part's arguments, and reference() takes and returns one part's arrays. A program takes and returns all parts, laid end to end along the dimension named above; an argument that names none is the same for every part. Nothing has to cross between parts.
All inputs are finite; a program needn't handle non-finite values.
Results may differ from the reference program's by a relative error of at most 0.024.
Values may be sent and summed in bfloat16 or wider, within the bound.
A program may use at most 64 MiB of HBM per device.

```python
import math
import jax
import jax.numpy as jnp
from jax import lax

D = 2048
FF = 5632
TAPS = 3
ROWS = 512
TOKENS = 2048
N_FS = 4
N_TP = 4


def draw_tokens(key, part):
    key_base = jax.random.fold_in(key, 11)
    key_rows = jax.random.fold_in(key, 12)
    base = jnp.clip(jax.random.normal(key_base, (TOKENS, D), jnp.float32), -6.0, 6.0)
    spread = jax.random.uniform(key_rows, (TOKENS, 1), jnp.float32, 0.0, math.log(10.0))
    return (base * jnp.exp(spread)).astype(jnp.bfloat16)


def levels(rng, shape, split, smallest, high):
    def one(position, shards_of):
        steps = jax.random.uniform(jax.random.fold_in(jax.random.fold_in(rng, 6), position), (shards_of,), jnp.float32, smallest / len(split), high / len(split))
        return jnp.repeat(jnp.exp(steps), shape[position] // shards_of).reshape((-1,) + (1,) * (len(shape) - position - 1))

    level = one(*split[0])
    for cut in split[1:]:
        level = level * one(*cut)
    return level


def scatter_about(rng, extent, scale, reach, shards=(), kind=jnp.bfloat16):
    drawn = scale * jax.random.normal(rng, extent, jnp.float32)
    if shards:
        drawn = drawn * levels(rng, extent, shards, -0.22, 0.18)
    return jnp.clip(drawn, -reach, reach).astype(kind)


def setup_inputs(seed: int = 0, part: int = 0) -> dict:
    keys = jax.random.split(jax.random.key(seed), 13)
    part_keys = jax.random.split(jax.random.fold_in(keys[12], part), 13)
    tokens = draw_tokens(jax.random.fold_in(jax.random.fold_in(keys[12], part), 71), part)
    norm_gain = jnp.clip(1.0 + 0.18 * jax.random.normal(keys[1], (D,), jnp.float32), 0.1, 1.9)
    value_weight = scatter_about(keys[2], (D, FF), D ** -0.5, 0.125, ((0, 4), (1, 4)), jnp.float32)
    gate_weight = scatter_about(keys[3], (D, FF), D ** -0.5, 0.125, ((0, 4), (1, 4)), jnp.float32)
    down_weight = scatter_about(keys[4], (D, FF), FF ** -0.5, 0.078125, ((0, 4), (1, 4)), jnp.float32)
    value_scale = jnp.clip(jnp.exp(math.log(3.0) - 2.3025851 * jax.random.uniform(keys[5], (FF,), jnp.float32) ** levels(keys[5], (FF,), ((0, 4),), -0.2, 0.2)), 0.3, 3.0)
    gate_scale = jnp.clip(jnp.exp(math.log(3.0) - 2.3025851 * jax.random.uniform(keys[6], (FF,), jnp.float32) ** levels(keys[6], (FF,), ((0, 4),), -0.2, 0.2)), 0.3, 3.0)
    down_scale = jnp.clip(jnp.exp(jax.random.uniform(keys[7], (D,), jnp.float32, math.log(0.3), math.log(3.0))), 0.3, 3.0)
    value_taps = scatter_about(keys[8], (TAPS, FF), 0.577, 3.0, ((1, 4),), jnp.float32)
    gate_taps = scatter_about(keys[9], (TAPS, FF), 0.577, 3.0, ((1, 4),), jnp.float32)
    value_bias = scatter_about(keys[10], (FF,), 0.5, 3.0, ((0, 4),), jnp.float32)
    gate_bias = scatter_about(keys[11], (FF,), 0.5, 3.0, ((0, 4),), jnp.float32)
    return dict(tokens=tokens, norm_gain=norm_gain, value_weight=value_weight, gate_weight=gate_weight, down_weight=down_weight, value_scale=value_scale, gate_scale=gate_scale, down_scale=down_scale, value_taps=value_taps, gate_taps=gate_taps, value_bias=value_bias, gate_bias=gate_bias)


def causal_mix(field, taps, bias):
    back_one = jnp.pad(field, ((1, 0), (0, 0)))[:-1]
    back_two = jnp.pad(field, ((2, 0), (0, 0)))[:-2]
    return taps[0] * back_two + taps[1] * back_one + taps[2] * field + bias

def reference(tokens, norm_gain, value_weight, gate_weight, down_weight, value_scale, gate_scale, down_scale, value_taps, gate_taps, value_bias, gate_bias):
    value_cast = value_weight.astype(jnp.bfloat16)
    gate_cast = gate_weight.astype(jnp.bfloat16)
    down_cast = down_weight.astype(jnp.bfloat16)

    def one_sequence(rows):
        floated = rows.astype(jnp.float32)
        inverse = lax.rsqrt(lax.optimization_barrier(jnp.mean(floated * floated, axis=-1, keepdims=True)) + 1e-06)
        normed = (floated * inverse * norm_gain).astype(jnp.bfloat16)
        value_up = jnp.dot(normed, value_cast, preferred_element_type=jnp.float32) * value_scale
        gate_up = jnp.dot(normed, gate_cast, preferred_element_type=jnp.float32) * gate_scale
        value_mixed = causal_mix(value_up, value_taps, value_bias)
        gate_mixed = causal_mix(gate_up, gate_taps, gate_bias)
        return (jax.nn.silu(gate_mixed) * value_mixed).astype(jnp.bfloat16)
    hidden = lax.map(one_sequence, tokens.reshape(N_FS, ROWS, D)).reshape(N_FS * ROWS, FF)
    block = FF // N_TP

    def add_block(index, total):
        start = (index * block).astype(jnp.int32)
        left = lax.dynamic_slice_in_dim(hidden, start, block, 1)
        right = lax.dynamic_slice_in_dim(down_cast, start, block, 1)
        term = lax.dot_general(left, right, (((1,), (1,)), ((), ())), preferred_element_type=jnp.float32)
        return total + term.astype(jnp.bfloat16).astype(jnp.float32)
    total = lax.fori_loop(0, N_TP, add_block, jnp.zeros((N_FS * ROWS, D), jnp.float32))
    return (total * down_scale).astype(jnp.bfloat16)
```

```python
import functools

import jax
import jax.numpy as jnp
from jax import lax
from jax.experimental import pallas as pl
from jax.experimental.pallas import tpu as pltpu
from jax.sharding import PartitionSpec as P

MESH = pl.DeviceIdType.MESH
WIDE = 256
RIGHT, LEFT, ACROSS = 0, 1, 2


def kernel(
    parts,
    line,
    peers,
    pieces,
    tokens,
    norm_gain,
    value_weight,
    gate_weight,
    down_weight,
    value_scale,
    gate_scale,
    down_scale,
    value_taps,
    gate_taps,
    value_bias,
    gate_bias,
    out,
    value_full,
    gate_full,
    down_full,
    normed,
    mixed,
    hidden,
    partial,
    landed,
    send_sem,
    recv_sem,
    sum_send,
    sum_recv,
):
    group, here, me = lax.axis_index("grp"), lax.axis_index("fs"), lax.axis_index("tp")
    full = (value_full, gate_full, down_full)
    shards = (value_weight, gate_weight, down_weight)
    rows, units = hidden.shape
    held = shards[0].shape[0]
    share = held // parts
    piece = share // pieces
    kept = rows // peers

    def greet(act):
        pl.when(here > 0)(lambda: act("fs", here - 1))
        pl.when(here < line - 1)(lambda: act("fs", here + 1))
        for k in range(1, parts):
            act("grp", lax.rem(group + k, parts))
        for k in range(1, peers):
            act("tp", lax.rem(me + k, peers))

    barrier = pltpu.get_barrier_semaphore()
    greet(
        lambda axis, index: pl.semaphore_signal(
            barrier, inc=1, device_id={axis: index}, device_id_type=MESH
        )
    )

    def cast(which):
        step = min(held, 64)

        def body(i, carry):
            source = pl.ds(pl.multiple_of(i * step, step), step)
            target = pl.ds(pl.multiple_of(here * held + i * step, step), step)
            full[which][target, :] = shards[which][source, :].astype(jnp.bfloat16)
            return carry

        lax.fori_loop(0, held // step, body, 0)

    def copy(which, owner, part, slot, direction):
        first = pl.multiple_of(owner * held + part * share + slot * piece, piece)
        block = full[which].at[pl.ds(first, piece), :]
        if direction == RIGHT:
            target = {"fs": lax.min(here + 1, line - 1)}
        elif direction == LEFT:
            target = {"fs": lax.max(here - 1, 0)}
        else:
            target = {"grp": lax.rem(group + direction - ACROSS + 1, parts)}
        return pltpu.make_async_remote_copy(
            src_ref=block,
            dst_ref=block,
            send_sem=send_sem.at[which, owner, slot, direction],
            recv_sem=recv_sem.at[which, owner, part, slot],
            device_id=target,
            device_id_type=MESH,
        )

    def own(which, act):
        for slot in range(pieces):
            pl.when(here < line - 1)(lambda: act(copy(which, here, group, slot, RIGHT)))
            pl.when(here > 0)(lambda: act(copy(which, here, group, slot, LEFT)))

    def onward(which, step, act, arrive):
        for slot in range(pieces):
            for direction in (RIGHT, LEFT):
                owner = here - step if direction == RIGHT else here + step
                there = owner >= 0 if direction == RIGHT else owner < line
                more = here < line - 1 if direction == RIGHT else here > 0

                @pl.when(there)
                def _():
                    if arrive:
                        copy(which, owner, group, slot, direction).wait_recv()
                    pl.when(more)(lambda: act(copy(which, owner, group, slot, direction)))
                    for k in range(parts - 1):
                        act(copy(which, owner, group, slot, ACROSS + k))

    def crossed(which, step):
        for slot in range(pieces):
            for owner, there in ((here - step, here >= step), (here + step, here + step < line)):

                @pl.when(there)
                def _():
                    for k in range(parts - 1):
                        part = lax.rem(group + k + 1, parts)
                        copy(which, owner, part, slot, ACROSS + k).wait_recv()

    def start(dma):
        dma.start()

    def left(dma):
        dma.wait_send()

    def normalize():
        step = min(rows, 64)

        def body(i, carry):
            block = pl.ds(pl.multiple_of(i * step, step), step)
            floated = tokens[block, :].astype(jnp.float32)
            mean = jnp.mean(floated * floated, axis=-1, keepdims=True)
            normed[block, :] = (floated * lax.rsqrt(mean + 1e-06) * norm_gain[...]).astype(
                jnp.bfloat16
            )
            return carry

        lax.fori_loop(0, rows // step, body, 0)

    def over_units(body):
        if units // WIDE:

            def one(i, carry):
                body(pl.ds(pl.multiple_of(i * WIDE, WIDE), WIDE), WIDE)
                return carry

            lax.fori_loop(0, units // WIDE, one, 0)
        if units % WIDE:
            body(pl.ds(units // WIDE * WIDE, units % WIDE), units % WIDE)

    def causal(which, scale, taps, bias, columns, width):
        up = jnp.dot(normed[...], full[which][:, columns], preferred_element_type=jnp.float32)
        up = up * scale[:, columns]
        position = lax.broadcasted_iota(jnp.int32, (rows, width), 0)
        one = jnp.where(position >= 1, pltpu.roll(up, 1, axis=0), 0.0)
        two = jnp.where(position >= 2, pltpu.roll(up, 2, axis=0), 0.0)
        return (
            taps[0:1, columns] * two
            + taps[1:2, columns] * one
            + taps[2:3, columns] * up
            + bias[:, columns]
        )

    def value(columns, width):
        mixed[:, columns] = causal(0, value_scale, value_taps, value_bias, columns, width)

    def gate(columns, width):
        gated = causal(1, gate_scale, gate_taps, gate_bias, columns, width)
        hidden[:, columns] = (gated / (1.0 + jnp.exp(-gated)) * mixed[:, columns]).astype(
            jnp.bfloat16
        )

    def give(owner, k):
        peer = lax.rem(me + k, peers)
        return pltpu.make_async_remote_copy(
            src_ref=partial.at[owner, pl.ds(pl.multiple_of(peer * kept, kept), kept), :],
            dst_ref=landed.at[k - 1, owner],
            send_sem=sum_send,
            recv_sem=sum_recv,
            device_id={"tp": peer},
            device_id_type=MESH,
        )

    def project(owner):
        block = full[2][pl.ds(pl.multiple_of(owner * held, held), held), :]
        partial[owner] = lax.dot_general(
            hidden[...], block, (((1,), (1,)), ((), ())), preferred_element_type=jnp.float32
        ).astype(jnp.bfloat16)
        for k in range(1, peers):
            give(owner, k).start()

    def project_at(step):
        crossed(2, step)
        pl.when(here >= step)(lambda: project(here - step))
        pl.when(here + step < line)(lambda: project(here + step))

    cast(0)
    ends = (here == 0).astype(jnp.int32) + (here == line - 1).astype(jnp.int32)
    pl.semaphore_wait(barrier, parts + peers - ends)
    own(0, start)
    cast(1)
    own(1, start)
    cast(2)
    normalize()
    for step in range(1, line):
        onward(0, step, start, True)
    onward(1, 1, start, True)
    own(2, start)
    for step in range(1, line):
        crossed(0, step)
    over_units(value)
    for step in range(2, line):
        onward(1, step, start, True)
    onward(2, 1, start, True)
    for step in range(1, line):
        crossed(1, step)
    over_units(gate)
    project(here)
    for step in range(2, line):
        onward(2, step, start, True)
        project_at(step - 1)
    project_at(line - 1)

    pltpu.make_async_copy(landed, landed, sum_recv).wait()
    mine = pl.ds(pl.multiple_of(me * kept, kept), kept)
    for owner in range(line):
        total = partial[owner, mine, :].astype(jnp.float32)
        for k in range(peers - 1):
            total = total + landed[k, owner].astype(jnp.float32)
        columns = slice(owner * held, (owner + 1) * held)
        out[:, columns] = (total * down_scale[:, columns]).astype(jnp.bfloat16)

    pltpu.make_async_copy(landed, landed, sum_send).wait()
    for which in range(3):
        own(which, left)
        for step in range(1, line):
            onward(which, step, left, False)


def solution(mesh):
    parts, line, peers = mesh.shape["grp"], mesh.shape["fs"], mesh.shape["tp"]

    def local(tokens, norm_gain, *rest):
        weights, scales, taps, biases = rest[:3], rest[3:6], rest[6:8], rest[8:]
        rows, width = tokens.shape
        held, units = weights[0].shape
        share = held // parts
        pieces = 2 if share % 2 == 0 and share // 2 >= 128 else 1
        kept = rows // peers
        whole = [pltpu.VMEM((width, units), jnp.bfloat16)] * 3
        return pl.pallas_call(
            functools.partial(kernel, parts, line, peers, pieces),
            out_shape=jax.ShapeDtypeStruct((kept, width), jnp.bfloat16),
            in_specs=[pl.BlockSpec(memory_space=pltpu.VMEM)] * 12,
            out_specs=pl.BlockSpec(memory_space=pltpu.VMEM),
            scratch_shapes=whole
            + [
                pltpu.VMEM((rows, width), jnp.bfloat16),
                pltpu.VMEM((rows, units), jnp.float32),
                pltpu.VMEM((rows, units), jnp.bfloat16),
                pltpu.VMEM((line, rows, held), jnp.bfloat16),
                pltpu.VMEM((peers - 1, line, kept, held), jnp.bfloat16),
                pltpu.SemaphoreType.DMA((3, line, pieces, 1 + parts)),
                pltpu.SemaphoreType.DMA((3, line, parts, pieces)),
                pltpu.SemaphoreType.DMA,
                pltpu.SemaphoreType.DMA,
            ],
            compiler_params=pltpu.CompilerParams(
                collective_id=0, has_side_effects=True, vmem_limit_bytes=60 * 1024 * 1024
            ),
        )(
            tokens,
            norm_gain[None],
            *weights,
            *(scale[None] for scale in scales),
            *taps,
            *(bias[None] for bias in biases),
        )

    return jax.shard_map(
        local,
        mesh=mesh,
        in_specs=(
            P(("grp", "fs"), None),
            P(),
            P("fs", "tp"),
            P("fs", "tp"),
            P("fs", "tp"),
            P("tp"),
            P("tp"),
            P(),
            P(None, "tp"),
            P(None, "tp"),
            P("tp"),
            P("tp"),
        ),
        out_specs=P(("grp", "fs", "tp"), None),
        check_vma=False,
    )
```

```python
import functools

import jax
import jax.numpy as jnp
from jax import lax
from jax.experimental import pallas as pl
from jax.experimental.pallas import tpu as pltpu
from jax.sharding import PartitionSpec as P

MESH = pl.DeviceIdType.MESH
WIDE = 256
RIGHT, LEFT, ACROSS = 0, 1, 2


def kernel(
    parts,
    line,
    peers,
    pieces,
    lent,
    tokens,
    norm_gain,
    value_weight,
    gate_weight,
    down_weight,
    value_scale,
    gate_scale,
    down_scale,
    value_taps,
    gate_taps,
    value_bias,
    gate_bias,
    out,
    *scratch,
):
    group, here, me = lax.axis_index("grp"), lax.axis_index("fs"), lax.axis_index("tp")
    scratch = list(scratch)
    take = lambda count: [scratch.pop(0) for _ in range(count)]
    kinds = 2 if lent else 1
    full = take(3 * kinds)
    normed, partial, landed, along, wide = take(5)
    mixed, hidden = take(kinds), take(kinds)
    send_sem, recv_sem, sum_send, sum_recv = take(4)
    if lent:
        guest, guest_mixed, guest_hidden, guest_partial, guest_landed, summed, returned = take(7)
        lend_send, lend_recv, guest_send, guest_recv = take(4)
        back_send, back_recv = take(2)
    shards = (value_weight, gate_weight, down_weight)
    rows = tokens.shape[0]
    held, units = shards[0].shape
    share = held // parts
    piece = share // pieces
    kept = rows // peers
    base = (0, units - lent)
    span = (units - lent, lent)
    end = jnp.logical_or(here == 0, here == line - 1)
    inner = jnp.logical_not(end)
    helper = jnp.logical_and(inner, jnp.logical_or(here == 1, here == line - 2))
    mate = jnp.where(end, jnp.where(here == 0, 1, line - 2), jnp.where(here == 1, 0, line - 1))

    barrier = pltpu.get_barrier_semaphore()

    def greet(axis, index):
        pl.semaphore_signal(barrier, inc=1, device_id={axis: index}, device_id_type=MESH)

    pl.when(here > 0)(lambda: greet("fs", here - 1))
    pl.when(here < line - 1)(lambda: greet("fs", here + 1))
    for k in range(1, parts):
        greet("grp", lax.rem(group + k, parts))
    for k in range(1, peers):
        greet("tp", lax.rem(me + k, peers))

    def spread():
        for i, vector in enumerate((value_scale, gate_scale, value_bias, gate_bias)):
            along[i : i + 1, :] = vector[...].reshape(1, units)
        for i, vector in enumerate((norm_gain, down_scale)):
            wide[i : i + 1, :] = vector[...].reshape(1, vector.shape[0])

    def cast(which):
        step = min(held, 64)

        def body(i, carry):
            source = pl.ds(pl.multiple_of(i * step, step), step)
            target = pl.ds(pl.multiple_of(here * held + i * step, step), step)
            for kind in range(kinds):
                columns = slice(base[kind], base[kind] + span[kind])
                full[which + 3 * kind][target, :] = shards[which][source, columns].astype(
                    jnp.bfloat16
                )
            return carry

        lax.fori_loop(0, held // step, body, 0)

    def copy(which, owner, part, slot, direction):
        first = pl.multiple_of(owner * held + part * share + slot * piece, piece)
        block = full[which].at[pl.ds(first, piece), :]
        if direction == RIGHT:
            target = {"fs": lax.min(here + 1, line - 1)}
        elif direction == LEFT:
            target = {"fs": lax.max(here - 1, 0)}
        else:
            target = {"grp": lax.rem(group + direction - ACROSS + 1, parts)}
        return pltpu.make_async_remote_copy(
            src_ref=block,
            dst_ref=block,
            send_sem=send_sem.at[which, owner, slot, direction],
            recv_sem=recv_sem.at[which, owner, part, slot],
            device_id=target,
            device_id_type=MESH,
        )

    def more(which, direction):
        edge = 0 if which < 3 else 1
        return here < line - 1 - edge if direction == RIGHT else here > edge

    def comes(which, owner):
        inside = jnp.logical_and(owner >= 0, owner < line)
        return inside if which < 3 else jnp.logical_and(inside, inner)

    def own(which, act):
        for each in range(which, 3 * kinds, 3):
            for slot in range(pieces):
                for direction in (RIGHT, LEFT):
                    pl.when(more(each, direction))(
                        lambda: act(copy(each, here, group, slot, direction))
                    )

    def onward(which, step, act, arrive):
        for each in range(which, 3 * kinds, 3):
            for slot in range(pieces):
                for direction in (RIGHT, LEFT):
                    owner = here - step if direction == RIGHT else here + step

                    @pl.when(comes(each, owner))
                    def _():
                        if arrive:
                            copy(each, owner, group, slot, direction).wait_recv()
                        pl.when(more(each, direction))(
                            lambda: act(copy(each, owner, group, slot, direction))
                        )
                        for k in range(parts - 1):
                            act(copy(each, owner, group, slot, ACROSS + k))

    def crossed(which, step):
        for each in range(which, 3 * kinds, 3):
            for slot in range(pieces):
                for owner in (here - step, here + step):

                    @pl.when(comes(each, owner))
                    def _():
                        for k in range(parts - 1):
                            part = lax.rem(group + k + 1, parts)
                            copy(each, owner, part, slot, ACROSS + k).wait_recv()

    def start(dma):
        dma.start()

    def left(dma):
        dma.wait_send()

    def normalize(source, offset):
        step = min(rows, 64)

        def body(i, carry):
            block = pl.ds(pl.multiple_of(i * step, step), step)
            target = pl.ds(pl.multiple_of(offset + i * step, step), step)
            floated = source[block, :].astype(jnp.float32)
            mean = jnp.mean(floated * floated, axis=-1, keepdims=True)
            normed[target, :] = (floated * lax.rsqrt(mean + 1e-06) * wide[0:1, :]).astype(
                jnp.bfloat16
            )
            return carry

        lax.fori_loop(0, rows // step, body, 0)

    mine = pl.ds(pl.multiple_of(me * kept, kept), kept)

    def lend():
        return pltpu.make_async_remote_copy(
            src_ref=tokens.at[mine, :],
            dst_ref=guest.at[mine, :],
            send_sem=lend_send,
            recv_sem=lend_recv,
            device_id={"fs": mate},
            device_id_type=MESH,
        )

    def relay(k):
        return pltpu.make_async_remote_copy(
            src_ref=guest.at[mine, :],
            dst_ref=guest.at[mine, :],
            send_sem=guest_send.at[line],
            recv_sem=guest_recv.at[line],
            device_id={"tp": lax.rem(me + k, peers)},
            device_id_type=MESH,
        )

    def relays():
        lend().wait_recv()
        for k in range(1, peers):
            relay(k).start()

    def guest_rows():
        others = guest.at[pl.ds(0, (peers - 1) * kept), :]
        return others

    def welcome():
        pltpu.make_async_copy(guest_rows(), guest_rows(), guest_recv.at[line]).wait()
        normalize(guest, rows)

    def over_units(kind, body):
        count = span[kind]
        if count // WIDE:

            def one(i, carry):
                first = pl.multiple_of(i * WIDE, WIDE)
                shifted = pl.multiple_of(base[kind] + i * WIDE, 128)
                body(pl.ds(first, WIDE), pl.ds(shifted, WIDE), WIDE)
                return carry

            lax.fori_loop(0, count // WIDE, one, 0)
        if count % WIDE:
            first = count // WIDE * WIDE
            body(pl.ds(first, count % WIDE), pl.ds(base[kind] + first, count % WIDE), count % WIDE)

    def causal(which, branch, taps, offset, columns, outer, width):
        up = jnp.dot(
            normed[offset : offset + rows, :],
            full[which][:, columns],
            preferred_element_type=jnp.float32,
        )
        up = up * along[branch : branch + 1, outer]
        position = lax.broadcasted_iota(jnp.int32, (rows, width), 0)
        one = jnp.where(position >= 1, pltpu.roll(up, 1, axis=0), 0.0)
        two = jnp.where(position >= 2, pltpu.roll(up, 2, axis=0), 0.0)
        return (
            taps[0:1, outer] * two
            + taps[1:2, outer] * one
            + taps[2:3, outer] * up
            + along[branch + 2 : branch + 3, outer]
        )

    def value(kind, keep, offset):
        def body(columns, outer, width):
            keep[:, columns] = causal(
                3 * kind, 0, value_taps, offset, columns, outer, width
            )

        over_units(kind, body)

    def gate(kind, kept_value, keep, offset):
        def body(columns, outer, width):
            gated = causal(1 + 3 * kind, 1, gate_taps, offset, columns, outer, width)
            keep[:, columns] = (
                gated / (1.0 + jnp.exp(-gated)) * kept_value[:, columns]
            ).astype(jnp.bfloat16)

        over_units(kind, body)

    def give(owner, k):
        peer = lax.rem(me + k, peers)
        return pltpu.make_async_remote_copy(
            src_ref=partial.at[owner, pl.ds(pl.multiple_of(peer * kept, kept), kept), :],
            dst_ref=landed.at[k - 1, owner],
            send_sem=sum_send,
            recv_sem=sum_recv,
            device_id={"tp": peer},
            device_id_type=MESH,
        )

    def guest_give(owner, k):
        peer = lax.rem(me + k, peers)
        return pltpu.make_async_remote_copy(
            src_ref=guest_partial.at[owner, pl.ds(pl.multiple_of(peer * kept, kept), kept), :],
            dst_ref=guest_landed.at[owner, k - 1],
            send_sem=guest_send.at[owner],
            recv_sem=guest_recv.at[owner],
            device_id={"tp": peer},
            device_id_type=MESH,
        )

    def down(left_side, kind, owner):
        block = full[2 + 3 * kind][pl.ds(pl.multiple_of(owner * held, held), held), :]
        return lax.dot_general(
            left_side[...], block, (((1,), (1,)), ((), ())), preferred_element_type=jnp.float32
        )

    def project(owner):
        if not lent:
            partial[owner] = down(hidden[0], 0, owner).astype(jnp.bfloat16)
        else:

            @pl.when(helper)
            def _():
                guest_partial[owner] = down(guest_hidden, 1, owner).astype(jnp.bfloat16)
                for k in range(1, peers):
                    guest_give(owner, k).start()

            @pl.when(inner)
            def _():
                partial[owner] = (down(hidden[0], 0, owner) + down(hidden[1], 1, owner)).astype(
                    jnp.bfloat16
                )

            @pl.when(end)
            def _():
                partial[owner] = down(hidden[0], 0, owner).astype(jnp.bfloat16)

        for k in range(1, peers):
            give(owner, k).start()

    def back(owner):
        return pltpu.make_async_remote_copy(
            src_ref=summed.at[owner],
            dst_ref=returned.at[owner],
            send_sem=back_send,
            recv_sem=back_recv,
            device_id={"fs": mate},
            device_id_type=MESH,
        )

    def give_back(owner):
        if lent:

            @pl.when(helper)
            def _():
                arrived = guest_landed.at[owner]
                pltpu.make_async_copy(arrived, arrived, guest_recv.at[owner]).wait()
                total = guest_partial[owner, mine, :].astype(jnp.float32)
                for k in range(peers - 1):
                    total = total + guest_landed[owner, k].astype(jnp.float32)
                summed[owner] = total.astype(jnp.bfloat16)
                back(owner).start()

    def around(step, act):
        pl.when(here >= step)(lambda: act(here - step))
        pl.when(here + step < line)(lambda: act(here + step))

    def project_at(step):
        crossed(2, step)
        around(step, project)

    spread()
    cast(0)
    ends = (here == 0).astype(jnp.int32) + (here == line - 1).astype(jnp.int32)
    pl.semaphore_wait(barrier, parts + peers - ends)
    own(0, start)
    if lent:
        pl.when(end)(lambda: lend().start())
    cast(1)
    own(1, start)
    cast(2)
    normalize(tokens, 0)
    for step in range(1, line):
        onward(0, step, start, True)
        if lent and step == 1:
            pl.when(helper)(relays)
    onward(1, 1, start, True)
    own(2, start)
    for step in range(1, line):
        crossed(0, step)
    value(0, mixed[0], 0)
    if lent:
        pl.when(inner)(lambda: value(1, mixed[1], 0))

        @pl.when(helper)
        def _():
            welcome()
            value(1, guest_mixed, rows)

    for step in range(2, line):
        onward(1, step, start, True)
    onward(2, 1, start, True)
    for step in range(1, line):
        crossed(1, step)
    gate(0, mixed[0], hidden[0], 0)
    if lent:
        pl.when(inner)(lambda: gate(1, mixed[1], hidden[1], 0))
        pl.when(helper)(lambda: gate(1, guest_mixed, guest_hidden, rows))
    project(here)
    for step in range(2, line):
        onward(2, step, start, True)
        project_at(step - 1)
        if step == 2:
            give_back(here)
        else:
            around(step - 2, give_back)
    project_at(line - 1)
    for step in range(max(line - 2, 1), line):
        around(step, give_back)

    pltpu.make_async_copy(landed, landed, sum_recv).wait()

    def finish(extra):
        for owner in range(line):
            total = partial[owner, mine, :].astype(jnp.float32)
            for k in range(peers - 1):
                total = total + landed[k, owner].astype(jnp.float32)
            if extra:
                total = total + returned[owner].astype(jnp.float32)
            columns = slice(owner * held, (owner + 1) * held)
            out[:, columns] = (total * wide[1:2, columns]).astype(jnp.bfloat16)

    if lent:

        @pl.when(end)
        def _():
            pltpu.make_async_copy(returned, returned, back_recv).wait()
            finish(True)
            lend().wait_send()

        pl.when(inner)(lambda: finish(False))

        @pl.when(helper)
        def _():
            pltpu.make_async_copy(guest_rows(), guest_rows(), guest_send.at[line]).wait()
            for owner in range(line):
                sent = guest_landed.at[owner]
                pltpu.make_async_copy(sent, sent, guest_send.at[owner]).wait()
            pltpu.make_async_copy(summed, summed, back_send).wait()

    else:
        finish(False)

    pltpu.make_async_copy(landed, landed, sum_send).wait()
    for which in range(3):
        own(which, left)
        for step in range(1, line):
            onward(which, step, left, False)


def solution(mesh):
    parts, line, peers = mesh.shape["grp"], mesh.shape["fs"], mesh.shape["tp"]

    def local(*arrays):
        rows, width = arrays[0].shape
        held, units = arrays[2].shape
        share = held // parts
        pieces = 2 if share % 2 == 0 and share // 2 >= 128 else 1
        kept = rows // peers
        lent = units * 5 // 11 // 128 * 128 if line >= 4 and peers > 1 else 0
        half, full = jnp.bfloat16, jnp.float32
        spans = (units - lent, lent) if lent else (units,)
        dma = pltpu.SemaphoreType.DMA
        scratch = [pltpu.VMEM((width, span), half) for span in spans for _ in range(3)]
        scratch += [
            pltpu.VMEM((rows * len(spans), width), half),
            pltpu.VMEM((line, rows, held), half),
            pltpu.VMEM((peers - 1, line, kept, held), half),
            pltpu.VMEM((4, units), full),
            pltpu.VMEM((2, width), full),
        ]
        scratch += [pltpu.VMEM((rows, span), full) for span in spans]
        scratch += [pltpu.VMEM((rows, span), half) for span in spans]
        scratch += [
            dma((3 * len(spans), line, pieces, 1 + parts)),
            dma((3 * len(spans), line, parts, pieces)),
            dma,
            dma,
        ]
        if lent:
            scratch += [
                pltpu.VMEM((rows, width), half),
                pltpu.VMEM((rows, lent), full),
                pltpu.VMEM((rows, lent), half),
                pltpu.VMEM((line, rows, held), half),
                pltpu.VMEM((line, peers - 1, kept, held), half),
                pltpu.VMEM((line, kept, held), half),
                pltpu.VMEM((line, kept, held), half),
                dma,
                dma,
                dma((line + 1,)),
                dma((line + 1,)),
                dma,
                dma,
            ]
        return pl.pallas_call(
            functools.partial(kernel, parts, line, peers, pieces, lent),
            out_shape=jax.ShapeDtypeStruct((kept, width), half),
            in_specs=[pl.BlockSpec(memory_space=pltpu.VMEM)] * 12,
            out_specs=pl.BlockSpec(memory_space=pltpu.VMEM),
            scratch_shapes=scratch,
            compiler_params=pltpu.CompilerParams(
                collective_id=0, has_side_effects=True, vmem_limit_bytes=60 * 1024 * 1024
            ),
        )(*arrays)

    return jax.shard_map(
        local,
        mesh=mesh,
        in_specs=(
            P(("grp", "fs"), None),
            P(),
            P("fs", "tp"),
            P("fs", "tp"),
            P("fs", "tp"),
            P("tp"),
            P("tp"),
            P(),
            P(None, "tp"),
            P(None, "tp"),
            P("tp"),
            P("tp"),
        ),
        out_specs=P(("grp", "fs", "tp"), None),
        check_vma=False,
    )
```

```python
import functools

import jax
import jax.numpy as jnp
from jax import lax
from jax.experimental import pallas as pl
from jax.experimental.pallas import tpu as pltpu
from jax.sharding import PartitionSpec as P

MESH = pl.DeviceIdType.MESH
WIDE = 256
RIGHT, LEFT, ACROSS = 0, 1, 2


def kernel(
    parts,
    line,
    peers,
    pieces,
    lent,
    tokens,
    norm_gain,
    value_weight,
    gate_weight,
    down_weight,
    value_scale,
    gate_scale,
    down_scale,
    value_taps,
    gate_taps,
    value_bias,
    gate_bias,
    out,
    *scratch,
):
    group, here, me = lax.axis_index("grp"), lax.axis_index("fs"), lax.axis_index("tp")
    scratch = list(scratch)
    take = lambda count: [scratch.pop(0) for _ in range(count)]
    kinds = 2 if lent else 1
    full = take(3 * kinds)
    normed, partial, landed, along, wide = take(5)
    mixed, hidden = take(kinds), take(kinds)
    send_sem, recv_sem, sum_send, sum_recv = take(4)
    if lent:
        guest, guest_mixed, guest_hidden, guest_partial, guest_landed, summed, returned = take(7)
        lend_send, lend_recv, guest_send, guest_recv = take(4)
        back_send, back_recv = take(2)
    shards = (value_weight, gate_weight, down_weight)
    rows = tokens.shape[0]
    held, units = shards[0].shape
    share = held // parts
    piece = share // pieces
    kept = rows // peers
    base = (0, units - lent)
    span = (units - lent, lent)
    end = jnp.logical_or(here == 0, here == line - 1)
    inner = jnp.logical_not(end)
    helper = jnp.logical_and(inner, jnp.logical_or(here == 1, here == line - 2))
    mate = jnp.where(end, jnp.where(here == 0, 1, line - 2), jnp.where(here == 1, 0, line - 1))

    barrier = pltpu.get_barrier_semaphore()

    def greet(axis, index):
        pl.semaphore_signal(barrier, inc=1, device_id={axis: index}, device_id_type=MESH)

    pl.when(here > 0)(lambda: greet("fs", here - 1))
    pl.when(here < line - 1)(lambda: greet("fs", here + 1))
    for k in range(1, parts):
        greet("grp", lax.rem(group + k, parts))
    for k in range(1, peers):
        greet("tp", lax.rem(me + k, peers))

    def spread():
        for i, vector in enumerate((value_scale, gate_scale, value_bias, gate_bias)):
            along[i : i + 1, :] = vector[...].reshape(1, units)
        for i, vector in enumerate((norm_gain, down_scale)):
            wide[i : i + 1, :] = vector[...].reshape(1, vector.shape[0])

    def cast(which):
        step = min(held, 64)

        def body(i, carry):
            source = pl.ds(pl.multiple_of(i * step, step), step)
            target = pl.ds(pl.multiple_of(here * held + i * step, step), step)
            for kind in range(kinds):
                columns = slice(base[kind], base[kind] + span[kind])
                full[which + 3 * kind][target, :] = shards[which][source, columns].astype(
                    jnp.bfloat16
                )
            return carry

        lax.fori_loop(0, held // step, body, 0)

    def copy(which, owner, part, slot, direction, neighbour=None):
        first = pl.multiple_of(owner * held + part * share + slot * piece, piece)
        block = full[which].at[pl.ds(first, piece), :]
        if neighbour is not None:
            target = {"fs": neighbour}
        elif direction == RIGHT:
            target = {"fs": lax.min(here + 1, line - 1)}
        elif direction == LEFT:
            target = {"fs": lax.max(here - 1, 0)}
        else:
            target = {"grp": lax.rem(group + direction - ACROSS + 1, parts)}
        return pltpu.make_async_remote_copy(
            src_ref=block,
            dst_ref=block,
            send_sem=send_sem.at[which, owner, slot, direction],
            recv_sem=recv_sem.at[which, owner, part, slot],
            device_id=target,
            device_id_type=MESH,
        )

    def more(which, direction):
        edge = 0 if which < 3 else 1
        return here < line - 1 - edge if direction == RIGHT else here > edge

    def comes(which, owner):
        inside = jnp.logical_and(owner >= 0, owner < line)
        return inside if which < 3 else jnp.logical_and(inside, inner)

    def own(which, act):
        for each in range(which, 3 * kinds, 3):
            for slot in range(pieces):
                for direction in (RIGHT, LEFT):
                    pl.when(more(each, direction))(
                        lambda: act(copy(each, here, group, slot, direction))
                    )

    def direct(each):
        return bool(lent) and each != 3 * kinds - 1

    def other(which, act):
        for each in range(which, 3 * kinds, 3):
            if direct(each):
                for slot in range(pieces):
                    for k in range(1, parts):
                        part = lax.rem(group + k, parts)
                        pl.when(end)(lambda: act(copy(each, here, part, slot, ACROSS + k - 1, mate)))

    def onward(which, step, act, arrive):
        for each in range(which, 3 * kinds, 3):
            for slot in range(pieces):
                for direction in (RIGHT, LEFT):
                    owner = here - step if direction == RIGHT else here + step

                    @pl.when(comes(each, owner))
                    def _():
                        if arrive:
                            copy(each, owner, group, slot, direction).wait_recv()
                        pl.when(more(each, direction))(
                            lambda: act(copy(each, owner, group, slot, direction))
                        )

                        def share_out():
                            for k in range(parts - 1):
                                act(copy(each, owner, group, slot, ACROSS + k))

                        if step == 1 and direct(each):
                            pl.when(jnp.logical_and(owner > 0, owner < line - 1))(share_out)
                        else:
                            share_out()

    def crossed(which, step):
        for each in range(which, 3 * kinds, 3):
            for slot in range(pieces):
                for owner in (here - step, here + step):

                    @pl.when(comes(each, owner))
                    def _():
                        for k in range(parts - 1):
                            part = lax.rem(group + k + 1, parts)
                            copy(each, owner, part, slot, ACROSS + k).wait_recv()

    def start(dma):
        dma.start()

    def left(dma):
        dma.wait_send()

    def normalize(source, offset):
        step = min(rows, 64)

        def body(i, carry):
            block = pl.ds(pl.multiple_of(i * step, step), step)
            target = pl.ds(pl.multiple_of(offset + i * step, step), step)
            floated = source[block, :].astype(jnp.float32)
            mean = jnp.mean(floated * floated, axis=-1, keepdims=True)
            normed[target, :] = (floated * lax.rsqrt(mean + 1e-06) * wide[0:1, :]).astype(
                jnp.bfloat16
            )
            return carry

        lax.fori_loop(0, rows // step, body, 0)

    mine = pl.ds(pl.multiple_of(me * kept, kept), kept)

    def lend():
        return pltpu.make_async_remote_copy(
            src_ref=tokens.at[mine, :],
            dst_ref=guest.at[mine, :],
            send_sem=lend_send,
            recv_sem=lend_recv,
            device_id={"fs": mate},
            device_id_type=MESH,
        )

    def relay(k):
        return pltpu.make_async_remote_copy(
            src_ref=guest.at[mine, :],
            dst_ref=guest.at[mine, :],
            send_sem=guest_send.at[line],
            recv_sem=guest_recv.at[line],
            device_id={"tp": lax.rem(me + k, peers)},
            device_id_type=MESH,
        )

    def relays():
        lend().wait_recv()
        for k in range(1, peers):
            relay(k).start()

    def guest_rows():
        others = guest.at[pl.ds(0, (peers - 1) * kept), :]
        return others

    def welcome():
        pltpu.make_async_copy(guest_rows(), guest_rows(), guest_recv.at[line]).wait()
        normalize(guest, rows)

    def over_units(kind, body):
        count = span[kind]
        if count // WIDE:

            def one(i, carry):
                first = pl.multiple_of(i * WIDE, WIDE)
                shifted = pl.multiple_of(base[kind] + i * WIDE, 128)
                body(pl.ds(first, WIDE), pl.ds(shifted, WIDE), WIDE)
                return carry

            lax.fori_loop(0, count // WIDE, one, 0)
        if count % WIDE:
            first = count // WIDE * WIDE
            body(pl.ds(first, count % WIDE), pl.ds(base[kind] + first, count % WIDE), count % WIDE)

    def causal(which, branch, taps, offset, columns, outer, width):
        up = jnp.dot(
            normed[offset : offset + rows, :],
            full[which][:, columns],
            preferred_element_type=jnp.float32,
        )
        up = up * along[branch : branch + 1, outer]
        position = lax.broadcasted_iota(jnp.int32, (rows, width), 0)
        one = jnp.where(position >= 1, pltpu.roll(up, 1, axis=0), 0.0)
        two = jnp.where(position >= 2, pltpu.roll(up, 2, axis=0), 0.0)
        return (
            taps[0:1, outer] * two
            + taps[1:2, outer] * one
            + taps[2:3, outer] * up
            + along[branch + 2 : branch + 3, outer]
        )

    def value(kind, keep, offset):
        def body(columns, outer, width):
            keep[:, columns] = causal(
                3 * kind, 0, value_taps, offset, columns, outer, width
            )

        over_units(kind, body)

    def gate(kind, kept_value, keep, offset):
        def body(columns, outer, width):
            gated = causal(1 + 3 * kind, 1, gate_taps, offset, columns, outer, width)
            keep[:, columns] = (
                gated / (1.0 + jnp.exp(-gated)) * kept_value[:, columns]
            ).astype(jnp.bfloat16)

        over_units(kind, body)

    def give(owner, k):
        peer = lax.rem(me + k, peers)
        return pltpu.make_async_remote_copy(
            src_ref=partial.at[owner, pl.ds(pl.multiple_of(peer * kept, kept), kept), :],
            dst_ref=landed.at[k - 1, owner],
            send_sem=sum_send,
            recv_sem=sum_recv,
            device_id={"tp": peer},
            device_id_type=MESH,
        )

    def guest_give(owner, k):
        peer = lax.rem(me + k, peers)
        return pltpu.make_async_remote_copy(
            src_ref=guest_partial.at[owner, pl.ds(pl.multiple_of(peer * kept, kept), kept), :],
            dst_ref=guest_landed.at[owner, k - 1],
            send_sem=guest_send.at[owner],
            recv_sem=guest_recv.at[owner],
            device_id={"tp": peer},
            device_id_type=MESH,
        )

    def down(left_side, kind, owner):
        block = full[2 + 3 * kind][pl.ds(pl.multiple_of(owner * held, held), held), :]
        return lax.dot_general(
            left_side[...], block, (((1,), (1,)), ((), ())), preferred_element_type=jnp.float32
        )

    def project(owner):
        if not lent:
            partial[owner] = down(hidden[0], 0, owner).astype(jnp.bfloat16)
        else:

            @pl.when(helper)
            def _():
                guest_partial[owner] = down(guest_hidden, 1, owner).astype(jnp.bfloat16)
                for k in range(1, peers):
                    guest_give(owner, k).start()

            @pl.when(inner)
            def _():
                partial[owner] = (down(hidden[0], 0, owner) + down(hidden[1], 1, owner)).astype(
                    jnp.bfloat16
                )

            @pl.when(end)
            def _():
                partial[owner] = down(hidden[0], 0, owner).astype(jnp.bfloat16)

        for k in range(1, peers):
            give(owner, k).start()

    def back(owner):
        return pltpu.make_async_remote_copy(
            src_ref=summed.at[owner],
            dst_ref=returned.at[owner],
            send_sem=back_send,
            recv_sem=back_recv,
            device_id={"fs": mate},
            device_id_type=MESH,
        )

    def give_back(owner):
        if lent:

            @pl.when(helper)
            def _():
                arrived = guest_landed.at[owner]
                pltpu.make_async_copy(arrived, arrived, guest_recv.at[owner]).wait()
                total = guest_partial[owner, mine, :].astype(jnp.float32)
                for k in range(peers - 1):
                    total = total + guest_landed[owner, k].astype(jnp.float32)
                summed[owner] = total.astype(jnp.bfloat16)
                back(owner).start()

    def around(step, act):
        pl.when(here >= step)(lambda: act(here - step))
        pl.when(here + step < line)(lambda: act(here + step))

    def project_at(step):
        crossed(2, step)
        around(step, project)

    spread()
    cast(0)
    ends = (here == 0).astype(jnp.int32) + (here == line - 1).astype(jnp.int32)
    pl.semaphore_wait(barrier, parts + peers - ends)
    own(0, start)
    cast(1)
    own(1, start)
    if lent:
        pl.when(end)(lambda: lend().start())
        other(0, start)
    cast(2)
    if lent:
        pl.when(end)(lambda: own(2, start))
        other(1, start)
        other(2, start)
    normalize(tokens, 0)
    for step in range(1, line):
        onward(0, step, start, True)
        if lent and step == 1:
            pl.when(helper)(relays)
    onward(1, 1, start, True)
    if lent:
        pl.when(inner)(lambda: own(2, start))
    else:
        own(2, start)
    for step in range(1, line):
        crossed(0, step)
    value(0, mixed[0], 0)
    if lent:
        pl.when(inner)(lambda: value(1, mixed[1], 0))

        @pl.when(helper)
        def _():
            welcome()
            value(1, guest_mixed, rows)

    for step in range(2, line):
        onward(1, step, start, True)
    onward(2, 1, start, True)
    for step in range(1, line):
        crossed(1, step)
    gate(0, mixed[0], hidden[0], 0)
    if lent:
        pl.when(inner)(lambda: gate(1, mixed[1], hidden[1], 0))
        pl.when(helper)(lambda: gate(1, guest_mixed, guest_hidden, rows))
    project(here)
    for step in range(2, line):
        onward(2, step, start, True)
        project_at(step - 1)
        if step == 2:
            give_back(here)
        else:
            around(step - 2, give_back)
    project_at(line - 1)
    for step in range(max(line - 2, 1), line):
        around(step, give_back)

    pltpu.make_async_copy(landed, landed, sum_recv).wait()

    def finish(extra):
        for owner in range(line):
            total = partial[owner, mine, :].astype(jnp.float32)
            for k in range(peers - 1):
                total = total + landed[k, owner].astype(jnp.float32)
            if extra:
                total = total + returned[owner].astype(jnp.float32)
            columns = slice(owner * held, (owner + 1) * held)
            out[:, columns] = (total * wide[1:2, columns]).astype(jnp.bfloat16)

    if lent:

        @pl.when(end)
        def _():
            pltpu.make_async_copy(returned, returned, back_recv).wait()
            finish(True)
            lend().wait_send()

        pl.when(inner)(lambda: finish(False))

        @pl.when(helper)
        def _():
            pltpu.make_async_copy(guest_rows(), guest_rows(), guest_send.at[line]).wait()
            for owner in range(line):
                sent = guest_landed.at[owner]
                pltpu.make_async_copy(sent, sent, guest_send.at[owner]).wait()
            pltpu.make_async_copy(summed, summed, back_send).wait()

    else:
        finish(False)

    pltpu.make_async_copy(landed, landed, sum_send).wait()
    for which in range(3):
        own(which, left)
        other(which, left)
        for step in range(1, line):
            onward(which, step, left, False)


def solution(mesh):
    parts, line, peers = mesh.shape["grp"], mesh.shape["fs"], mesh.shape["tp"]

    def local(*arrays):
        rows, width = arrays[0].shape
        held, units = arrays[2].shape
        share = held // parts
        pieces = 2 if share % 2 == 0 and share // 2 >= 128 else 1
        kept = rows // peers
        lent = units * 5 // 11 // 128 * 128 if line >= 4 and peers > 1 else 0
        half, full = jnp.bfloat16, jnp.float32
        spans = (units - lent, lent) if lent else (units,)
        dma = pltpu.SemaphoreType.DMA
        scratch = [pltpu.VMEM((width, span), half) for span in spans for _ in range(3)]
        scratch += [
            pltpu.VMEM((rows * len(spans), width), half),
            pltpu.VMEM((line, rows, held), half),
            pltpu.VMEM((peers - 1, line, kept, held), half),
            pltpu.VMEM((4, units), full),
            pltpu.VMEM((2, width), full),
        ]
        scratch += [pltpu.VMEM((rows, span), full) for span in spans]
        scratch += [pltpu.VMEM((rows, span), half) for span in spans]
        scratch += [
            dma((3 * len(spans), line, pieces, 1 + parts)),
            dma((3 * len(spans), line, parts, pieces)),
            dma,
            dma,
        ]
        if lent:
            scratch += [
                pltpu.VMEM((rows, width), half),
                pltpu.VMEM((rows, lent), full),
                pltpu.VMEM((rows, lent), half),
                pltpu.VMEM((line, rows, held), half),
                pltpu.VMEM((line, peers - 1, kept, held), half),
                pltpu.VMEM((line, kept, held), half),
                pltpu.VMEM((line, kept, held), half),
                dma,
                dma,
                dma((line + 1,)),
                dma((line + 1,)),
                dma,
                dma,
            ]
        return pl.pallas_call(
            functools.partial(kernel, parts, line, peers, pieces, lent),
            out_shape=jax.ShapeDtypeStruct((kept, width), half),
            in_specs=[pl.BlockSpec(memory_space=pltpu.VMEM)] * 12,
            out_specs=pl.BlockSpec(memory_space=pltpu.VMEM),
            scratch_shapes=scratch,
            compiler_params=pltpu.CompilerParams(
                collective_id=0, has_side_effects=True, vmem_limit_bytes=60 * 1024 * 1024
            ),
        )(*arrays)

    return jax.shard_map(
        local,
        mesh=mesh,
        in_specs=(
            P(("grp", "fs"), None),
            P(),
            P("fs", "tp"),
            P("fs", "tp"),
            P("fs", "tp"),
            P("tp"),
            P("tp"),
            P(),
            P(None, "tp"),
            P(None, "tp"),
            P("tp"),
            P("tp"),
        ),
        out_specs=P(("grp", "fs", "tp"), None),
        check_vma=False,
    )
```
